32 devices in a mesh: sp: 16 (over z, y, x), tp: 2 (over core).
Axes of the slice: x: 2, y: 2, z: 4, core: 2. Of those that a mesh axis runs over, the one named last changes fastest.
Arguments:
- stream: bfloat16 [7168, 2048], P('sp'), may hold values from -6 to 6
- norm_gain: float32 [2, 2048], replicated, may hold values from 0.1 to 1.9
- value_weight: bfloat16 [2, 2048, 512], P(None, None, 'tp'), may hold values from -0.125 to 0.125
- gate_weight: bfloat16 [2, 2048, 512], P(None, None, 'tp'), may hold values from -0.125 to 0.125
- conv_taps: bfloat16 [2, 512, 512], P(None, None, 'tp'), may hold values from -0.25 to 0.25
- conv_bias: float32 [2, 512], P(None, 'tp'), may hold values from -3 to 3
- channel_gain: float32 [2, 512], replicated, may hold values from 0.1 to 1.9
- channel_shift: float32 [2, 512], replicated, may hold values from -3 to 3
- out_weight: bfloat16 [2, 512, 2048], replicated, may hold values from -0.25 to 0.25
Outputs:
- result: bfloat16 [7168, 2048], P('sp')
The draws below stay inside these ranges and needn't reach their ends.
All inputs are finite; a program needn't handle non-finite values.
Results may differ from the reference program's by a relative error of at most 0.0075.
Values may be sent and summed in bfloat16 or wider, within the bound.
A program may use at most 64 MiB of HBM per device.

```python
import jax
import jax.numpy as jnp
from jax import lax

D = 2048
CH = 512
KW = 512
LAYERS = 2
TOKENS = 7168


def block_scale(key, shape, pieces, smallest, high):
    loudness, own = 1.0, jax.random.fold_in(key, 6)
    for dim, parts in pieces:
        steps = jnp.exp(jax.random.uniform(jax.random.fold_in(own, dim), (parts,), jnp.float32, smallest / len(pieces), high / len(pieces)))
        loudness = loudness * jnp.repeat(steps, shape[dim] // parts).reshape([-1 if axis == dim else 1 for axis in range(len(shape))])
    return loudness


def scatter_about(stream_key, dims, scale, most, split=(), held_as=jnp.bfloat16):
    array = scale * jax.random.normal(stream_key, dims, jnp.float32)
    if split:
        array = array * block_scale(stream_key, dims, split, -0.22, 0.18)
    return jnp.clip(array, -most, most).astype(held_as)


def setup_inputs(seed: int = 0) -> dict:
    key_list = jax.random.split(jax.random.key(seed), 10)
    stream = scatter_about(key_list[0], (TOKENS, D), 1.0, 6.0, ((0, 16),))
    norm_gain = jnp.clip(1.0 + 0.18 * jax.random.normal(key_list[1], (LAYERS, D), jnp.float32), 0.1, 1.9)
    value_weight = scatter_about(key_list[2], (LAYERS, D, CH), D ** -0.5, 0.125, ((2, 2),))
    gate_weight = scatter_about(key_list[3], (LAYERS, D, CH), D ** -0.5, 0.125, ((2, 2),))
    conv_taps = scatter_about(key_list[4], (LAYERS, KW, CH), KW ** -0.5, 0.25, ((2, 2),))
    conv_bias = scatter_about(key_list[5], (LAYERS, CH), 0.5, 3.0, ((1, 2),), jnp.float32)
    channel_gain = jnp.clip(1.0 + 0.18 * jax.random.normal(key_list[6], (LAYERS, CH), jnp.float32), 0.1, 1.9)
    channel_shift = scatter_about(key_list[7], (LAYERS, CH), 0.5, 3.0, (), jnp.float32)
    out_weight = scatter_about(key_list[8], (LAYERS, CH, D), CH ** -0.5, 0.25)
    return dict(stream=stream, norm_gain=norm_gain, value_weight=value_weight, gate_weight=gate_weight, conv_taps=conv_taps, conv_bias=conv_bias, channel_gain=channel_gain, channel_shift=channel_shift, out_weight=out_weight)


def rms_normed(stream, gain):
    values = stream.astype(jnp.float32)
    scale = lax.rsqrt(lax.optimization_barrier(jnp.mean(values * values, axis=-1, keepdims=True)) + 1e-06)
    return (values * scale * gain[None, :]).astype(jnp.bfloat16)

def channel_mix(conv, gain, shift):
    values = conv.astype(jnp.float32)
    center = lax.optimization_barrier(jnp.mean(values, axis=-1, keepdims=True))
    spread = lax.optimization_barrier(jnp.mean(jnp.square(values - center), axis=-1, keepdims=True))
    normed = (values - center) * lax.rsqrt(spread + 1e-05) * gain[None, :] + shift[None, :]
    return jax.nn.silu(normed).astype(jnp.bfloat16)

def causal_conv(gated, taps):
    length = gated.shape[0]
    span = taps.shape[0]
    padded_len = 1 << (length + span - 2).bit_length()
    signal = jnp.fft.rfft(gated.astype(jnp.float32), n=padded_len, axis=0)
    kernel = jnp.fft.rfft(taps.astype(jnp.float32)[::-1], n=padded_len, axis=0)
    return jnp.fft.irfft(signal * kernel, n=padded_len, axis=0)[:length]

def reference(stream, norm_gain, value_weight, gate_weight, conv_taps, conv_bias, channel_gain, channel_shift, out_weight):
    state = stream
    for layer in range(LAYERS):
        normed = rms_normed(state, norm_gain[layer])
        values = jnp.dot(normed, value_weight[layer], preferred_element_type=jnp.float32)
        gates = jnp.dot(normed, gate_weight[layer], preferred_element_type=jnp.float32)
        gated = (values * jax.nn.sigmoid(gates)).astype(jnp.bfloat16)
        conv = causal_conv(gated, conv_taps[layer])
        conv = (conv + conv_bias[layer][None, :]).astype(jnp.bfloat16)
        mixed = channel_mix(conv, channel_gain[layer], channel_shift[layer])
        update = jnp.dot(mixed, out_weight[layer], preferred_element_type=jnp.float32)
        state = (state.astype(jnp.float32) + update).astype(jnp.bfloat16)
    return state
```

```python
import jax
import numpy as np
import jax.numpy as jnp
from jax import lax
from jax.sharding import PartitionSpec as P


def passed_along(value, axis, by):
    count = lax.axis_size(axis)
    pairs = [(i, i + by) for i in range(count) if 0 <= i + by < count]
    return lax.ppermute(value, axis, pairs)


def rms_normed(stream, gain):
    values = stream.astype(jnp.float32)
    scale = lax.rsqrt(jnp.mean(values * values, axis=-1, keepdims=True) + 1e-06)
    return (values * scale * gain[None, :]).astype(jnp.bfloat16)


def channel_mix(conv, gain, shift):
    values = conv.astype(jnp.float32)
    center = jnp.mean(values, axis=-1, keepdims=True)
    spread = jnp.mean(jnp.square(values - center), axis=-1, keepdims=True)
    normed = (values - center) * lax.rsqrt(spread + 1e-05) * gain[None, :] + shift[None, :]
    return jax.nn.silu(normed).astype(jnp.bfloat16)


def gate_rows(normed, w_value, w_gate):
    values = jnp.dot(normed, w_value, preferred_element_type=jnp.float32)
    gates = jnp.dot(normed, w_gate, preferred_element_type=jnp.float32)
    return (values * jax.nn.sigmoid(gates)).astype(jnp.bfloat16)


BLOCK = 128


def dft_matrices(block):
    span = 2 * block
    angle = 2 * np.pi / span * np.outer(np.arange(block) + 0.5, np.arange(span))
    forward = np.concatenate([np.cos(angle), -np.sin(angle)], axis=0)
    of_taps = forward[:, block - 1 :: -1]
    inverse = forward[:, block:].T / block
    return [jnp.asarray(m, jnp.bfloat16) for m in (forward, of_taps, inverse)]


def long_conv(gated, taps, tokens):
    forward, of_taps, inverse = dft_matrices(BLOCK)
    parts = taps.shape[0] // BLOCK
    outs = -(-tokens // BLOCK)
    rows = (parts + outs) * BLOCK
    gated = jnp.pad(gated, ((rows - gated.shape[0], 0), (0, 0)))
    spectra = []
    for w in range(parts + outs - 1):
        window = gated[w * BLOCK : (w + 2) * BLOCK]
        spectra.append(jnp.dot(forward, window, preferred_element_type=jnp.float32))
    kernels = []
    for j in range(parts):
        part = taps[(parts - 1 - j) * BLOCK : (parts - j) * BLOCK]
        kernels.append(jnp.dot(of_taps, part, preferred_element_type=jnp.float32))
    results = []
    for p in range(outs):
        real = imag = 0.0
        for j in range(parts):
            x, h = spectra[parts - 1 + p - j], kernels[j]
            xr, xi, hr, hi = x[:BLOCK], x[BLOCK:], h[:BLOCK], h[BLOCK:]
            real = real + xr * hr - xi * hi
            imag = imag + xr * hi + xi * hr
        both = jnp.concatenate([real, imag], axis=0).astype(jnp.bfloat16)
        results.append(jnp.dot(inverse, both, preferred_element_type=jnp.float32))
    return jnp.concatenate(results, axis=0)[outs * BLOCK - tokens :]


def per_device(
    stream,
    norm_gain,
    value_weight,
    gate_weight,
    conv_taps,
    conv_bias,
    channel_gain,
    channel_shift,
    out_weight,
):
    tokens = stream.shape[0]
    reach = conv_taps.shape[1] - 1
    hops = -(-reach // tokens)
    state = stream
    for layer in range(norm_gain.shape[0]):
        normed = rms_normed(state, norm_gain[layer])
        own_gated = gate_rows(normed, value_weight[layer], gate_weight[layer])
        pieces = [own_gated]
        for step in range(1, hops + 1):
            count = min(tokens, reach - (step - 1) * tokens)
            pieces.insert(0, passed_along(own_gated[tokens - count :], "sp", step))
        gated = jnp.concatenate(pieces, axis=0)
        conv = long_conv(gated, conv_taps[layer], tokens)
        conv = (conv + conv_bias[layer][None, :]).astype(jnp.bfloat16)
        every_channel = lax.all_gather(conv, "tp", axis=1, tiled=True)
        mixed = channel_mix(every_channel, channel_gain[layer], channel_shift[layer])
        update = jnp.dot(mixed, out_weight[layer], preferred_element_type=jnp.float32)
        state = (state.astype(jnp.float32) + update).astype(jnp.bfloat16)
    return state


def solution(mesh):
    return jax.shard_map(
        per_device,
        mesh=mesh,
        in_specs=(
            P("sp", None),
            P(),
            P(None, None, "tp"),
            P(None, None, "tp"),
            P(None, None, "tp"),
            P(None, "tp"),
            P(),
            P(),
            P(),
        ),
        out_specs=P("sp", None),
        check_vma=False,
    )
```

```python
import functools

import jax
import jax.numpy as jnp
import numpy as np
from jax import lax
from jax.experimental import pallas as pl
from jax.experimental.pallas import tpu as pltpu
from jax.sharding import PartitionSpec as P

BLOCK = 128
MESH = pl.DeviceIdType.MESH


def dft_matrices(block):
    span = 2 * block
    angle = 2 * np.pi / span * np.outer(np.arange(block) + 0.5, np.arange(span))
    forward = np.concatenate([np.cos(angle), -np.sin(angle)], axis=0)
    of_taps = forward[:, block - 1 :: -1]
    inverse = forward[:, block:].T / block
    return [jnp.asarray(m, jnp.bfloat16) for m in (forward, of_taps, inverse)]


class Plan:
    def __init__(self, tokens, width, reach, n_sp):
        self.tokens, self.n_sp = tokens, n_sp
        self.parts = reach // BLOCK
        self.outs = -(-tokens // BLOCK)
        self.rows = (self.parts + self.outs) * BLOCK
        self.own = self.rows - tokens
        low = self.own - reach
        self.chunks = []
        for p in reversed(range(self.outs)):
            start = (self.parts + p) * BLOCK
            self.chunks.append((max(start, self.own), start + BLOCK))
        self.pieces = []
        for c, (a, b) in enumerate(self.chunks):
            for hop in range(1, min(-(-reach // tokens), n_sp - 1) + 1):
                first = max(a, low + hop * tokens)
                if first < b:
                    self.pieces.append((c, hop, first, first - hop * tokens, b - first))


def kernel(
    plan, layers, stream, gain, wv, wg, taps, bias, cgain, cshift, wo, fwd, oft, inv, out,
    x_v, gain_v, w_v, taps_v, bias_v, cgain_v, cshift_v, wo_v, fwd_v, oft_v, inv_v,
    gated, spectra, kernels, freq, conv, load_sem, out_sem, send_sem, recv_sem, swap_send, swap_recv,
):
    sp, tp = lax.axis_index("sp"), lax.axis_index("tp")
    half = wv.shape[2]
    loads = {}

    def load(name, source, target):
        copy = pltpu.make_async_copy(source, target, load_sem.at[len(loads)])
        loads[name] = copy
        copy.start()

    waited = set()

    def need(*names):
        for name in names:
            if name not in waited:
                waited.add(name)
                loads[name].wait()

    def own_rows(c):
        a, b = plan.chunks[c]
        return pl.ds(a - plan.own, b - a)

    load("gain", gain, gain_v)
    load(("x", 0), stream.at[own_rows(0)], x_v.at[own_rows(0)])
    load(("wv", 0), wv.at[0], w_v.at[0, :, pl.ds(0, half)])
    load(("wg", 0), wg.at[0], w_v.at[0, :, pl.ds(half, half)])
    for c in range(1, plan.outs):
        load(("x", c), stream.at[own_rows(c)], x_v.at[own_rows(c)])
    load("oft", oft, oft_v)
    load("taps", taps, taps_v)
    load("fwd", fwd, fwd_v)
    load("inv", inv, inv_v)
    load("bias", bias, bias_v)
    load("cgain", cgain, cgain_v)
    load("cshift", cshift, cshift_v)
    load(("wo", 0), wo.at[0], wo_v.at[0])
    for l in range(1, layers):
        load(("wv", l), wv.at[l], w_v.at[l, :, pl.ds(0, half)])
        load(("wg", l), wg.at[l], w_v.at[l, :, pl.ds(half, half)])
        load(("wo", l), wo.at[l], wo_v.at[l])

    for l in range(layers):
        gated[l, : plan.own] = jnp.zeros((plan.own, half), jnp.bfloat16)

    hops = sorted({piece[1] for piece in plan.pieces})
    barrier = pltpu.get_barrier_semaphore()
    pl.semaphore_signal(barrier, inc=1, device_id={"tp": 1 - tp}, device_id_type=MESH)
    for hop in hops:
        @pl.when(sp >= hop)
        def _():
            pl.semaphore_signal(barrier, inc=1, device_id={"sp": sp - hop}, device_id_type=MESH)
    pl.semaphore_wait(barrier, 1 + jnp.minimum(plan.n_sp - 1 - sp, len(hops)))

    def piece_copy(l, i):
        _, hop, source, target, count = plan.pieces[i]
        return pltpu.make_async_remote_copy(
            src_ref=gated.at[l, pl.ds(source, count)],
            dst_ref=gated.at[l, pl.ds(target, count)],
            send_sem=send_sem.at[l, i],
            recv_sem=recv_sem.at[l, i],
            device_id={"sp": sp + hop},
            device_id_type=MESH,
        )

    def swap_copy(l, c):
        part = conv.at[l, tp, own_rows(c)]
        return pltpu.make_async_remote_copy(
            src_ref=part,
            dst_ref=part,
            send_sem=swap_send.at[l, c],
            recv_sem=swap_recv.at[l, c],
            device_id={"tp": 1 - tp},
            device_id_type=MESH,
        )

    def gate(l, c):
        need("gain")
        if l == 0:
            need(("x", c))
        x = x_v[own_rows(c), :].astype(jnp.float32)
        scale = lax.rsqrt(jnp.mean(x * x, axis=-1, keepdims=True) + 1e-06)
        normed = (x * scale * gain_v[l : l + 1, :]).astype(jnp.bfloat16)
        need(("wv", l), ("wg", l))
        both = jnp.dot(normed, w_v[l], preferred_element_type=jnp.float32)
        a, b = plan.chunks[c]
        gated[l, a:b, :] = (both[:, :half] * jax.nn.sigmoid(both[:, half:])).astype(jnp.bfloat16)

    def send(l, c):
        for i, piece in enumerate(plan.pieces):
            if piece[0] == c:
                @pl.when(sp + piece[1] < plan.n_sp)
                def _():
                    piece_copy(l, i).start()

    def transform_taps(l):
        need("oft", "taps")
        for j in range(plan.parts):
            first = (plan.parts - 1 - j) * BLOCK
            kernels[l, j] = jnp.dot(
                oft_v[...], taps_v[l, first : first + BLOCK, :], preferred_element_type=jnp.float32
            )

    arrived = set()

    def spectrum(l, w):
        first, last = w * BLOCK, (w + 2) * BLOCK
        for i, (_, hop, _, target, count) in enumerate(plan.pieces):
            if (l, i) not in arrived and target < last and target + count > first:
                arrived.add((l, i))
                @pl.when(sp >= hop)
                def _():
                    piece_copy(l, i).wait_recv()
        need("fwd")
        spectra[w] = jnp.dot(fwd_v[...], gated[l, first:last, :], preferred_element_type=jnp.float32)

    def convolve(l, c):
        p = plan.outs - 1 - c
        tile = 16

        def bins(k, carry):
            low = pl.ds(pl.multiple_of(k * tile, tile), tile)
            high = pl.ds(pl.multiple_of(BLOCK + k * tile, tile), tile)
            real = imag = None
            for j in range(plan.parts):
                w = plan.parts - 1 + p - j
                xr, xi = spectra[w, low, :], spectra[w, high, :]
                hr, hi = kernels[l, j, low, :], kernels[l, j, high, :]
                r, i = xr * hr - xi * hi, xr * hi + xi * hr
                real, imag = (r, i) if real is None else (real + r, imag + i)
            freq[low, :] = real.astype(jnp.bfloat16)
            freq[high, :] = imag.astype(jnp.bfloat16)
            return carry

        lax.fori_loop(0, BLOCK // tile, bins, 0)
        need("inv", "bias")
        a, b = plan.chunks[c]
        result = jnp.dot(inv_v[BLOCK - (b - a) :, :], freq[...], preferred_element_type=jnp.float32)
        conv[l, tp, own_rows(c), :] = (result + bias_v[l : l + 1, :]).astype(jnp.bfloat16)
        swap_copy(l, c).start()

    def finish(l, c):
        rows = own_rows(c)
        swap_copy(l, c).wait()
        need("cgain", "cshift", ("wo", l))
        values = jnp.concatenate([conv[l, 0, rows, :], conv[l, 1, rows, :]], axis=-1).astype(jnp.float32)
        center = jnp.mean(values, axis=-1, keepdims=True)
        values = values - center
        spread = jnp.mean(values * values, axis=-1, keepdims=True)
        normed = values * lax.rsqrt(spread + 1e-05) * cgain_v[l : l + 1, :] + cshift_v[l : l + 1, :]
        mixed = (normed * jax.nn.sigmoid(normed)).astype(jnp.bfloat16)
        width = x_v.shape[1]
        step = width // 4
        for n in range(0, width, step):
            update = jnp.dot(mixed, wo_v[l, :, n : n + step], preferred_element_type=jnp.float32)
            old = x_v[rows, n : n + step].astype(jnp.float32)
            x_v[rows, n : n + step] = (old + update).astype(jnp.bfloat16)

    def write(c):
        return pltpu.make_async_copy(x_v.at[own_rows(c)], out.at[own_rows(c)], out_sem.at[c])

    for c in range(plan.outs):
        gate(0, c)
        send(0, c)
    for l in range(layers):
        transform_taps(l)
    for l in range(layers):
        last = l == layers - 1
        windows = plan.parts + plan.outs - 1
        done = windows

        def after(c):
            finish(l, c)
            if last:
                write(c).start()
            else:
                gate(l + 1, c)
                send(l + 1, c)

        for c in range(plan.outs):
            p = plan.outs - 1 - c
            while done > p:
                done -= 1
                spectrum(l, done)
            convolve(l, c)
            if c:
                after(c - 1)
        after(plan.outs - 1)

    for l in range(layers):
        for i, piece in enumerate(plan.pieces):
            @pl.when(sp + piece[1] < plan.n_sp)
            def _():
                piece_copy(l, i).wait_send()
    for c in range(plan.outs):
        write(c).wait()


def per_device(stream, norm_gain, value_weight, gate_weight, conv_taps, conv_bias, channel_gain, channel_shift, out_weight):
    tokens, width = stream.shape
    layers, reach, half = conv_taps.shape
    plan = Plan(tokens, width, reach, lax.axis_size("sp"))
    mats = dft_matrices(BLOCK)
    channels = out_weight.shape[1]
    n_pieces = len(plan.pieces)
    bf16, f32, dma = jnp.bfloat16, jnp.float32, pltpu.SemaphoreType.DMA
    windows = plan.parts + plan.outs - 1
    return pl.pallas_call(
        functools.partial(kernel, plan, layers),
        out_shape=jax.ShapeDtypeStruct(stream.shape, stream.dtype),
        in_specs=[pl.BlockSpec(memory_space=pl.ANY)] * 12,
        out_specs=pl.BlockSpec(memory_space=pl.ANY),
        scratch_shapes=[
            pltpu.VMEM((tokens, width), bf16),
            pltpu.VMEM(norm_gain.shape, f32),
            pltpu.VMEM((layers, width, 2 * half), bf16),
            pltpu.VMEM(conv_taps.shape, bf16),
            pltpu.VMEM(conv_bias.shape, f32),
            pltpu.VMEM(channel_gain.shape, f32),
            pltpu.VMEM(channel_shift.shape, f32),
            pltpu.VMEM(out_weight.shape, bf16),
            *[pltpu.VMEM(m.shape, bf16) for m in mats],
            pltpu.VMEM((layers, plan.rows, half), bf16),
            pltpu.VMEM((windows, 2 * BLOCK, half), f32),
            pltpu.VMEM((layers, plan.parts, 2 * BLOCK, half), f32),
            pltpu.VMEM((2 * BLOCK, half), bf16),
            pltpu.VMEM((layers, channels // half, tokens, half), bf16),
            dma((8 + plan.outs + 3 * layers,)),
            dma((plan.outs,)),
            dma((layers, n_pieces)),
            dma((layers, n_pieces)),
            dma((layers, plan.outs)),
            dma((layers, plan.outs)),
        ],
        compiler_params=pltpu.CompilerParams(
            collective_id=0, has_side_effects=True, vmem_limit_bytes=60000 * 1024
        ),
    )(stream, norm_gain, value_weight, gate_weight, conv_taps, conv_bias, channel_gain, channel_shift, out_weight, *mats)


def solution(mesh):
    return jax.shard_map(
        per_device,
        mesh=mesh,
        in_specs=(
            P("sp", None),
            P(),
            P(None, None, "tp"),
            P(None, None, "tp"),
            P(None, None, "tp"),
            P(None, "tp"),
            P(),
            P(),
            P(),
        ),
        out_specs=P("sp", None),
        check_vma=False,
    )
```

```python
import functools

import jax
import jax.numpy as jnp
import numpy as np
from jax import lax
from jax.experimental import pallas as pl
from jax.experimental.pallas import tpu as pltpu
from jax.sharding import PartitionSpec as P

BLOCK = 128
MESH = pl.DeviceIdType.MESH


def dft_matrices(block):
    span = 2 * block
    angle = 2 * np.pi / span * np.outer(np.arange(block) + 0.5, np.arange(span))
    forward = np.concatenate([np.cos(angle), -np.sin(angle)], axis=0)
    of_taps = forward[:, block - 1 :: -1]
    inverse = forward[:, block:].T / block
    return [jnp.asarray(m, jnp.bfloat16) for m in (forward, of_taps, inverse)]


class Plan:
    def __init__(self, tokens, width, reach, n_sp):
        self.tokens, self.n_sp = tokens, n_sp
        self.parts = reach // BLOCK
        self.outs = -(-tokens // BLOCK)
        self.rows = (self.parts + self.outs) * BLOCK
        self.own = self.rows - tokens
        low = self.own - reach
        self.chunks = []
        for p in reversed(range(self.outs)):
            start = (self.parts + p) * BLOCK
            self.chunks.append((max(start, self.own), start + BLOCK))
        self.pieces = []
        for c, (a, b) in enumerate(self.chunks):
            for hop in range(1, min(-(-reach // tokens), n_sp - 1) + 1):
                first = max(a, low + hop * tokens)
                if first < b:
                    self.pieces.append((c, hop, first, first - hop * tokens, b - first))


def kernel(
    plan, layers, stream, gain, wv, wg, taps, bias, cgain, cshift, wo, fwd, oft, inv, x_v,
    gain_v, w_v, taps_v, bias_v, cgain_v, cshift_v, wo_v, fwd_v, oft_v, inv_v,
    gated, spectra, kernels, freq, conv, load_sem, send_sem, recv_sem, swap_send, swap_recv,
):
    sp, tp = lax.axis_index("sp"), lax.axis_index("tp")
    half = wv.shape[2]
    loads = {}

    def load(name, source, target):
        copy = pltpu.make_async_copy(source, target, load_sem.at[len(loads)])
        loads[name] = copy
        copy.start()

    waited = set()

    def need(*names):
        for name in names:
            if name not in waited:
                waited.add(name)
                loads[name].wait()

    def own_rows(c):
        a, b = plan.chunks[c]
        return pl.ds(a - plan.own, b - a)

    load("gain", gain, gain_v)
    load(("x", 0), stream.at[own_rows(0)], x_v.at[own_rows(0)])
    load(("wv", 0), wv.at[0], w_v.at[0, :, pl.ds(0, half)])
    load(("wg", 0), wg.at[0], w_v.at[0, :, pl.ds(half, half)])
    for c in range(1, plan.outs):
        load(("x", c), stream.at[own_rows(c)], x_v.at[own_rows(c)])
    load("oft", oft, oft_v)
    load("taps", taps, taps_v)
    load("fwd", fwd, fwd_v)
    load("inv", inv, inv_v)
    load("bias", bias, bias_v)
    load("cgain", cgain, cgain_v)
    load("cshift", cshift, cshift_v)
    load(("wo", 0), wo.at[0], wo_v.at[0])
    for l in range(1, layers):
        load(("wv", l), wv.at[l], w_v.at[l, :, pl.ds(0, half)])
        load(("wg", l), wg.at[l], w_v.at[l, :, pl.ds(half, half)])
        load(("wo", l), wo.at[l], wo_v.at[l])

    for l in range(layers):
        gated[l, : plan.own] = jnp.zeros((plan.own, half), jnp.bfloat16)

    hops = sorted({piece[1] for piece in plan.pieces})
    barrier = pltpu.get_barrier_semaphore()
    pl.semaphore_signal(barrier, inc=1, device_id={"tp": 1 - tp}, device_id_type=MESH)
    for hop in hops:
        @pl.when(sp >= hop)
        def _():
            pl.semaphore_signal(barrier, inc=1, device_id={"sp": sp - hop}, device_id_type=MESH)
    pl.semaphore_wait(barrier, 1 + jnp.minimum(plan.n_sp - 1 - sp, len(hops)))

    def piece_copy(l, i):
        _, hop, source, target, count = plan.pieces[i]
        return pltpu.make_async_remote_copy(
            src_ref=gated.at[l, pl.ds(source, count)],
            dst_ref=gated.at[l, pl.ds(target, count)],
            send_sem=send_sem.at[l, i],
            recv_sem=recv_sem.at[l, i],
            device_id={"sp": sp + hop},
            device_id_type=MESH,
        )

    def swap_copy(l, c):
        part = conv.at[l, tp, own_rows(c)]
        return pltpu.make_async_remote_copy(
            src_ref=part,
            dst_ref=part,
            send_sem=swap_send.at[l, c],
            recv_sem=swap_recv.at[l, c],
            device_id={"tp": 1 - tp},
            device_id_type=MESH,
        )

    def gate(l, c):
        need("gain")
        if l == 0:
            need(("x", c))
        x = x_v[own_rows(c), :].astype(jnp.float32)
        scale = lax.rsqrt(jnp.mean(x * x, axis=-1, keepdims=True) + 1e-06)
        normed = (x * scale * gain_v[l : l + 1, :]).astype(jnp.bfloat16)
        need(("wv", l), ("wg", l))
        both = jnp.dot(normed, w_v[l], preferred_element_type=jnp.float32)
        a, b = plan.chunks[c]
        gated[l, a:b, :] = (both[:, :half] * jax.nn.sigmoid(both[:, half:])).astype(jnp.bfloat16)

    def send(l, c):
        for i, piece in enumerate(plan.pieces):
            if piece[0] == c:
                @pl.when(sp + piece[1] < plan.n_sp)
                def _():
                    piece_copy(l, i).start()

    def transform_taps(l):
        need("oft", "taps")
        for j in range(plan.parts):
            first = (plan.parts - 1 - j) * BLOCK
            kernels[l, j] = jnp.dot(
                oft_v[...], taps_v[l, first : first + BLOCK, :], preferred_element_type=jnp.float32
            )

    arrived = set()

    def spectrum(l, w):
        first, last = w * BLOCK, (w + 2) * BLOCK
        for i, (_, hop, _, target, count) in enumerate(plan.pieces):
            if (l, i) not in arrived and target < last and target + count > first:
                arrived.add((l, i))
                @pl.when(sp >= hop)
                def _():
                    piece_copy(l, i).wait_recv()
        need("fwd")
        spectra[w] = jnp.dot(fwd_v[...], gated[l, first:last, :], preferred_element_type=jnp.float32)

    def convolve(l, c):
        p = plan.outs - 1 - c
        tile = 16

        def bins(k, carry):
            low = pl.ds(pl.multiple_of(k * tile, tile), tile)
            high = pl.ds(pl.multiple_of(BLOCK + k * tile, tile), tile)
            real = imag = None
            for j in range(plan.parts):
                w = plan.parts - 1 + p - j
                xr, xi = spectra[w, low, :], spectra[w, high, :]
                hr, hi = kernels[l, j, low, :], kernels[l, j, high, :]
                r, i = xr * hr - xi * hi, xr * hi + xi * hr
                real, imag = (r, i) if real is None else (real + r, imag + i)
            freq[low, :] = real.astype(jnp.bfloat16)
            freq[high, :] = imag.astype(jnp.bfloat16)
            return carry

        lax.fori_loop(0, BLOCK // tile, bins, 0)
        need("inv", "bias")
        a, b = plan.chunks[c]
        result = jnp.dot(inv_v[BLOCK - (b - a) :, :], freq[...], preferred_element_type=jnp.float32)
        conv[l, tp, own_rows(c), :] = (result + bias_v[l : l + 1, :]).astype(jnp.bfloat16)
        swap_copy(l, c).start()

    def finish(l, c):
        rows = own_rows(c)
        swap_copy(l, c).wait()
        need("cgain", "cshift", ("wo", l))
        values = jnp.concatenate([conv[l, 0, rows, :], conv[l, 1, rows, :]], axis=-1).astype(jnp.float32)
        center = jnp.mean(values, axis=-1, keepdims=True)
        values = values - center
        spread = jnp.mean(values * values, axis=-1, keepdims=True)
        normed = values * lax.rsqrt(spread + 1e-05) * cgain_v[l : l + 1, :] + cshift_v[l : l + 1, :]
        mixed = (normed * jax.nn.sigmoid(normed)).astype(jnp.bfloat16)
        width = x_v.shape[1]
        step = width // 4
        for n in range(0, width, step):
            update = jnp.dot(mixed, wo_v[l, :, n : n + step], preferred_element_type=jnp.float32)
            old = x_v[rows, n : n + step].astype(jnp.float32)
            x_v[rows, n : n + step] = (old + update).astype(jnp.bfloat16)

    for c in range(plan.outs):
        gate(0, c)
        send(0, c)
    for l in range(layers):
        transform_taps(l)
    for l in range(layers):
        last = l == layers - 1
        windows = plan.parts + plan.outs - 1
        done = windows

        def after(c):
            finish(l, c)
            if not last:
                gate(l + 1, c)
                send(l + 1, c)

        for c in range(plan.outs):
            p = plan.outs - 1 - c
            while done > p:
                done -= 1
                spectrum(l, done)
            convolve(l, c)
            if c:
                after(c - 1)
        after(plan.outs - 1)

    for l in range(layers):
        for i, piece in enumerate(plan.pieces):
            @pl.when(sp + piece[1] < plan.n_sp)
            def _():
                piece_copy(l, i).wait_send()


def per_device(stream, norm_gain, value_weight, gate_weight, conv_taps, conv_bias, channel_gain, channel_shift, out_weight):
    tokens, width = stream.shape
    layers, reach, half = conv_taps.shape
    plan = Plan(tokens, width, reach, lax.axis_size("sp"))
    mats = dft_matrices(BLOCK)
    channels = out_weight.shape[1]
    n_pieces = len(plan.pieces)
    bf16, f32, dma = jnp.bfloat16, jnp.float32, pltpu.SemaphoreType.DMA
    windows = plan.parts + plan.outs - 1
    return pl.pallas_call(
        functools.partial(kernel, plan, layers),
        out_shape=pltpu.VMEM(stream.shape, stream.dtype),
        in_specs=[pl.BlockSpec(memory_space=pltpu.HBM)] * 12,
        out_specs=pl.BlockSpec(memory_space=pltpu.VMEM),
        scratch_shapes=[
            pltpu.VMEM(norm_gain.shape, f32),
            pltpu.VMEM((layers, width, 2 * half), bf16),
            pltpu.VMEM(conv_taps.shape, bf16),
            pltpu.VMEM(conv_bias.shape, f32),
            pltpu.VMEM(channel_gain.shape, f32),
            pltpu.VMEM(channel_shift.shape, f32),
            pltpu.VMEM(out_weight.shape, bf16),
            *[pltpu.VMEM(m.shape, bf16) for m in mats],
            pltpu.VMEM((layers, plan.rows, half), bf16),
            pltpu.VMEM((windows, 2 * BLOCK, half), f32),
            pltpu.VMEM((layers, plan.parts, 2 * BLOCK, half), f32),
            pltpu.VMEM((2 * BLOCK, half), bf16),
            pltpu.VMEM((layers, channels // half, tokens, half), bf16),
            dma((8 + plan.outs + 3 * layers,)),
            dma((layers, n_pieces)),
            dma((layers, n_pieces)),
            dma((layers, plan.outs)),
            dma((layers, plan.outs)),
        ],
        compiler_params=pltpu.CompilerParams(
            collective_id=0, has_side_effects=True, vmem_limit_bytes=40000 * 1024
        ),
    )(stream, norm_gain, value_weight, gate_weight, conv_taps, conv_bias, channel_gain, channel_shift, out_weight, *mats)


def solution(mesh):
    return jax.shard_map(
        per_device,
        mesh=mesh,
        in_specs=(
            P("sp", None),
            P(),
            P(None, None, "tp"),
            P(None, None, "tp"),
            P(None, None, "tp"),
            P(None, "tp"),
            P(),
            P(),
            P(),
        ),
        out_specs=P("sp", None),
        check_vma=False,
    )
```

```python
import functools

import jax
import jax.numpy as jnp
import numpy as np
from jax import lax
from jax.experimental import pallas as pl
from jax.experimental.pallas import tpu as pltpu
from jax.sharding import PartitionSpec as P

BLOCK = 128
MESH = pl.DeviceIdType.MESH


def dft_matrices(block):
    span = 2 * block
    angle = 2 * np.pi / span * np.outer(np.arange(block) + 0.5, np.arange(span))
    forward = np.concatenate([np.cos(angle), -np.sin(angle)], axis=0)
    of_taps = forward[:, block - 1 :: -1]
    inverse = forward[:, block:].T / block
    return [jnp.asarray(m, jnp.bfloat16) for m in (forward, of_taps, inverse)]


class Plan:
    def __init__(self, tokens, width, reach, n_sp):
        self.tokens, self.n_sp = tokens, n_sp
        self.parts = reach // BLOCK
        self.outs = -(-tokens // BLOCK)
        self.rows = (self.parts + self.outs) * BLOCK
        self.own = self.rows - tokens
        low = self.own - reach
        self.chunks = []
        for p in reversed(range(self.outs)):
            start = (self.parts + p) * BLOCK
            self.chunks.append((max(start, self.own), start + BLOCK))
        self.pieces = []
        for c, (a, b) in enumerate(self.chunks):
            for hop in range(1, min(-(-reach // tokens), n_sp - 1) + 1):
                first = max(a, low + hop * tokens)
                if first < b:
                    self.pieces.append((c, hop, first, first - hop * tokens, b - first))


def kernel(
    plan, layers, stream, gain, wv, wg, taps, bias, cgain, cshift, wo, fwd, oft, inv, x_v,
    gain_v, w_v, taps_v, bias_v, cgain_v, cshift_v, wo_v, fwd_v, oft_v, inv_v,
    gated, spectra, kernels, freq, conv, load_sem, send_sem, recv_sem, swap_send, swap_recv,
):
    sp, tp = lax.axis_index("sp"), lax.axis_index("tp")
    half = wv.shape[2]
    loads = {}

    def load(name, source, target):
        copy = pltpu.make_async_copy(source, target, load_sem.at[len(loads)])
        loads[name] = copy
        copy.start()

    waited = set()

    def need(*names):
        for name in names:
            if name not in waited:
                waited.add(name)
                loads[name].wait()

    def own_rows(c):
        a, b = plan.chunks[c]
        return pl.ds(a - plan.own, b - a)

    load("gain", gain, gain_v)
    load(("x", 0), stream.at[own_rows(0)], x_v.at[own_rows(0)])
    load(("wv", 0), wv.at[0], w_v.at[0, :, pl.ds(0, half)])
    load(("wg", 0), wg.at[0], w_v.at[0, :, pl.ds(half, half)])
    for c in range(1, plan.outs):
        load(("x", c), stream.at[own_rows(c)], x_v.at[own_rows(c)])
    load("oft", oft, oft_v)
    load("taps", taps, taps_v)
    load("fwd", fwd, fwd_v)
    load("inv", inv, inv_v)
    load("bias", bias, bias_v)
    load("cgain", cgain, cgain_v)
    load("cshift", cshift, cshift_v)
    load(("wo", 0), wo.at[0], wo_v.at[0])
    for l in range(1, layers):
        load(("wv", l), wv.at[l], w_v.at[l, :, pl.ds(0, half)])
        load(("wg", l), wg.at[l], w_v.at[l, :, pl.ds(half, half)])
        load(("wo", l), wo.at[l], wo_v.at[l])

    for l in range(layers):
        gated[l, : plan.own] = jnp.zeros((plan.own, half), jnp.bfloat16)

    hops = sorted({piece[1] for piece in plan.pieces})
    barrier = pltpu.get_barrier_semaphore()
    pl.semaphore_signal(barrier, inc=1, device_id={"tp": 1 - tp}, device_id_type=MESH)
    for hop in hops:
        @pl.when(sp >= hop)
        def _():
            pl.semaphore_signal(barrier, inc=1, device_id={"sp": sp - hop}, device_id_type=MESH)
    pl.semaphore_wait(barrier, 1 + jnp.minimum(plan.n_sp - 1 - sp, len(hops)))

    def piece_copy(l, i):
        _, hop, source, target, count = plan.pieces[i]
        return pltpu.make_async_remote_copy(
            src_ref=gated.at[l, pl.ds(source, count)],
            dst_ref=gated.at[l, pl.ds(target, count)],
            send_sem=send_sem.at[l, i],
            recv_sem=recv_sem.at[l, i],
            device_id={"sp": sp + hop},
            device_id_type=MESH,
        )

    def swap_copy(l, c):
        part = conv.at[l, tp, own_rows(c)]
        return pltpu.make_async_remote_copy(
            src_ref=part,
            dst_ref=part,
            send_sem=swap_send.at[l, c],
            recv_sem=swap_recv.at[l, c],
            device_id={"tp": 1 - tp},
            device_id_type=MESH,
        )

    def gate(l, c):
        need("gain")
        if l == 0:
            need(("x", c))
        x = x_v[own_rows(c), :].astype(jnp.float32)
        scale = lax.rsqrt(jnp.mean(x * x, axis=-1, keepdims=True) + 1e-06)
        normed = (x * scale * gain_v[l : l + 1, :]).astype(jnp.bfloat16)
        need(("wv", l), ("wg", l))
        both = jnp.dot(normed, w_v[l], preferred_element_type=jnp.float32)
        a, b = plan.chunks[c]
        gated[l, a:b, :] = (both[:, :half] * jax.nn.sigmoid(both[:, half:])).astype(jnp.bfloat16)

    def send(l, c):
        for i, piece in enumerate(plan.pieces):
            if piece[0] == c:
                @pl.when(sp + piece[1] < plan.n_sp)
                def _():
                    piece_copy(l, i).start()

    def transform_taps(l):
        need("oft", "taps")
        for j in range(plan.parts):
            first = (plan.parts - 1 - j) * BLOCK
            kernels[l, j] = jnp.dot(
                oft_v[...], taps_v[l, first : first + BLOCK, :], preferred_element_type=jnp.float32
            )

    arrived = set()

    def spectrum(l, w):
        first, last = w * BLOCK, (w + 2) * BLOCK
        for i, (_, hop, _, target, count) in enumerate(plan.pieces):
            if (l, i) not in arrived and target < last and target + count > first:
                arrived.add((l, i))
                @pl.when(sp >= hop)
                def _():
                    piece_copy(l, i).wait_recv()
        need("fwd")
        spectra[w] = jnp.dot(fwd_v[...], gated[l, first:last, :], preferred_element_type=jnp.float32)

    def convolve(l, c):
        p = plan.outs - 1 - c
        tile = 16

        def bins(k, carry):
            low = pl.ds(pl.multiple_of(k * tile, tile), tile)
            high = pl.ds(pl.multiple_of(BLOCK + k * tile, tile), tile)
            real = imag = None
            for j in range(plan.parts):
                w = plan.parts - 1 + p - j
                xr, xi = spectra[w, low, :], spectra[w, high, :]
                hr, hi = kernels[l, j, low, :], kernels[l, j, high, :]
                r, i = xr * hr - xi * hi, xr * hi + xi * hr
                real, imag = (r, i) if real is None else (real + r, imag + i)
            freq[low, :] = real.astype(jnp.bfloat16)
            freq[high, :] = imag.astype(jnp.bfloat16)
            return carry

        lax.fori_loop(0, BLOCK // tile, bins, 0)
        need("inv", "bias")
        a, b = plan.chunks[c]
        result = jnp.dot(inv_v[BLOCK - (b - a) :, :], freq[...], preferred_element_type=jnp.float32)
        conv[l, tp, own_rows(c), :] = (result + bias_v[l : l + 1, :]).astype(jnp.bfloat16)
        swap_copy(l, c).start()

    def finish(l, c):
        rows = own_rows(c)
        swap_copy(l, c).wait()
        need("cgain", "cshift", ("wo", l))
        values = jnp.concatenate([conv[l, 0, rows, :], conv[l, 1, rows, :]], axis=-1).astype(jnp.float32)
        center = jnp.mean(values, axis=-1, keepdims=True)
        values = values - center
        spread = jnp.mean(values * values, axis=-1, keepdims=True)
        normed = values * lax.rsqrt(spread + 1e-05) * cgain_v[l : l + 1, :] + cshift_v[l : l + 1, :]
        mixed = (normed * jax.nn.sigmoid(normed)).astype(jnp.bfloat16)
        width = x_v.shape[1]
        step = width // 4
        for n in range(0, width, step):
            update = jnp.dot(mixed, wo_v[l, :, n : n + step], preferred_element_type=jnp.float32)
            old = x_v[rows, n : n + step].astype(jnp.float32)
            x_v[rows, n : n + step] = (old + update).astype(jnp.bfloat16)

    for c in range(plan.outs):
        gate(0, c)
        send(0, c)
    for l in range(layers):
        transform_taps(l)
    for l in range(layers):
        last = l == layers - 1
        windows = plan.parts + plan.outs - 1
        done = windows

        def after(c):
            finish(l, c)
            if not last:
                gate(l + 1, c)
                send(l + 1, c)

        for c in range(plan.outs):
            p = plan.outs - 1 - c
            while done > p:
                done -= 1
                spectrum(l, done)
            convolve(l, c)
            if c:
                after(c - 1)
        after(plan.outs - 1)

    for l in range(layers):
        for i, piece in enumerate(plan.pieces):
            @pl.when(sp + piece[1] < plan.n_sp)
            def _():
                piece_copy(l, i).wait_send()


def per_device(stream, norm_gain, value_weight, gate_weight, conv_taps, conv_bias, channel_gain, channel_shift, out_weight):
    tokens, width = stream.shape
    layers, reach, half = conv_taps.shape
    plan = Plan(tokens, width, reach, lax.axis_size("sp"))
    mats = dft_matrices(BLOCK)
    channels = out_weight.shape[1]
    n_pieces = len(plan.pieces)
    bf16, f32, dma = jnp.bfloat16, jnp.float32, pltpu.SemaphoreType.DMA
    windows = plan.parts + plan.outs - 1
    return pl.pallas_call(
        functools.partial(kernel, plan, layers),
        out_shape=pltpu.VMEM(stream.shape, stream.dtype),
        in_specs=[pl.BlockSpec(memory_space=pltpu.HBM)] * 12,
        out_specs=pl.BlockSpec(memory_space=pltpu.VMEM),
        scratch_shapes=[
            pltpu.VMEM(norm_gain.shape, f32),
            pltpu.VMEM((layers, width, 2 * half), bf16),
            pltpu.VMEM(conv_taps.shape, bf16),
            pltpu.VMEM(conv_bias.shape, f32),
            pltpu.VMEM(channel_gain.shape, f32),
            pltpu.VMEM(channel_shift.shape, f32),
            pltpu.VMEM(out_weight.shape, bf16),
            *[pltpu.VMEM(m.shape, bf16) for m in mats],
            pltpu.VMEM((layers, plan.rows, half), bf16),
            pltpu.VMEM((windows, 2 * BLOCK, half), f32),
            pltpu.VMEM((layers, plan.parts, 2 * BLOCK, half), f32),
            pltpu.VMEM((2 * BLOCK, half), bf16),
            pltpu.VMEM((layers, channels // half, tokens, half), bf16),
            dma((8 + plan.outs + 3 * layers,)),
            dma((layers, n_pieces)),
            dma((layers, n_pieces)),
            dma((layers, plan.outs)),
            dma((layers, plan.outs)),
        ],
        compiler_params=pltpu.CompilerParams(
            collective_id=0, has_side_effects=True, vmem_limit_bytes=60000 * 1024
        ),
    )(stream, norm_gain, value_weight, gate_weight, conv_taps, conv_bias, channel_gain, channel_shift, out_weight, *mats)


def solution(mesh):
    return jax.shard_map(
        per_device,
        mesh=mesh,
        in_specs=(
            P("sp", None),
            P(),
            P(None, None, "tp"),
            P(None, None, "tp"),
            P(None, None, "tp"),
            P(None, "tp"),
            P(),
            P(),
            P(),
        ),
        out_specs=P("sp", None),
        check_vma=False,
    )
```

```python
import functools

import jax
import jax.numpy as jnp
import numpy as np
from jax import lax
from jax.experimental import pallas as pl
from jax.experimental.pallas import tpu as pltpu
from jax.sharding import PartitionSpec as P

BLOCK = 128
MESH = pl.DeviceIdType.MESH


def dft_matrices(block):
    span = 2 * block
    angle = 2 * np.pi / span * np.outer(np.arange(block) + 0.5, np.arange(span))
    forward = np.concatenate([np.cos(angle), -np.sin(angle)], axis=0)
    of_taps = forward[:, block - 1 :: -1]
    inverse = forward[:, block:].T / block
    return [jnp.asarray(m, jnp.bfloat16) for m in (forward, of_taps, inverse)]


class Plan:
    def __init__(self, tokens, width, reach, n_sp):
        self.tokens, self.n_sp = tokens, n_sp
        self.parts = reach // BLOCK
        self.outs = -(-tokens // BLOCK)
        self.rows = (self.parts + self.outs) * BLOCK
        self.own = self.rows - tokens
        low = self.own - reach
        self.chunks = []
        for p in reversed(range(self.outs)):
            start = (self.parts + p) * BLOCK
            self.chunks.append((max(start, self.own), start + BLOCK))
        self.pieces = []
        for c, (a, b) in enumerate(self.chunks):
            for hop in range(1, min(-(-reach // tokens), n_sp - 1) + 1):
                first, end = max(a, low + hop * tokens) - hop * tokens, b - hop * tokens
                while first < end:
                    cut = max(first, (end - 1) // BLOCK * BLOCK if end <= self.outs * BLOCK else first)
                    when = c if hop == 1 else max(c, self.outs - 2)
                    self.pieces.append((when, hop, cut + hop * tokens, cut, end - cut))
                    end = cut
        self.pieces.sort(key=lambda piece: piece[:2])


def kernel(
    plan, layers, stream, gain, wv, wg, taps, bias, cgain, cshift, wo, fwd, oft, inv, x_v,
    gain_v, w_v, taps_v, bias_v, cgain_v, cshift_v, wo_v, fwd_v, oft_v, inv_v,
    gated, spectra, kernels, freq, conv, load_sem, send_sem, recv_sem, swap_send, swap_recv,
):
    sp, tp = lax.axis_index("sp"), lax.axis_index("tp")
    half = wv.shape[2]
    loads = {}

    def load(name, source, target):
        copy = pltpu.make_async_copy(source, target, load_sem.at[len(loads)])
        loads[name] = copy
        copy.start()

    waited = set()

    def need(*names):
        for name in names:
            if name not in waited:
                waited.add(name)
                loads[name].wait()

    def own_rows(c):
        a, b = plan.chunks[c]
        return pl.ds(a - plan.own, b - a)

    load("gain", gain, gain_v)
    load(("x", 0), stream.at[own_rows(0)], x_v.at[own_rows(0)])
    load(("wv", 0), wv.at[0], w_v.at[0, :, pl.ds(0, half)])
    load(("wg", 0), wg.at[0], w_v.at[0, :, pl.ds(half, half)])
    for c in range(1, plan.outs):
        load(("x", c), stream.at[own_rows(c)], x_v.at[own_rows(c)])
    load("oft", oft, oft_v)
    load("taps", taps, taps_v)
    load("fwd", fwd, fwd_v)
    load("inv", inv, inv_v)
    load("bias", bias, bias_v)
    load("cgain", cgain, cgain_v)
    load("cshift", cshift, cshift_v)
    load(("wo", 0), wo.at[0], wo_v.at[0])
    for l in range(1, layers):
        load(("wv", l), wv.at[l], w_v.at[l, :, pl.ds(0, half)])
        load(("wg", l), wg.at[l], w_v.at[l, :, pl.ds(half, half)])
        load(("wo", l), wo.at[l], wo_v.at[l])

    for l in range(layers):
        gated[l, : plan.own] = jnp.zeros((plan.own, half), jnp.bfloat16)

    hops = sorted({piece[1] for piece in plan.pieces})
    barrier = pltpu.get_barrier_semaphore()
    pl.semaphore_signal(barrier, inc=1, device_id={"tp": 1 - tp}, device_id_type=MESH)
    for hop in hops:
        @pl.when(sp >= hop)
        def _():
            pl.semaphore_signal(barrier, inc=1, device_id={"sp": sp - hop}, device_id_type=MESH)

    def piece_copy(l, i):
        _, hop, source, target, count = plan.pieces[i]
        return pltpu.make_async_remote_copy(
            src_ref=gated.at[l, pl.ds(source, count)],
            dst_ref=gated.at[l, pl.ds(target, count)],
            send_sem=send_sem.at[l, i],
            recv_sem=recv_sem.at[l, i],
            device_id={"sp": sp + hop},
            device_id_type=MESH,
        )

    def swap_copy(l, c):
        part = conv.at[l, tp, own_rows(c)]
        return pltpu.make_async_remote_copy(
            src_ref=part,
            dst_ref=part,
            send_sem=swap_send.at[l, c],
            recv_sem=swap_recv.at[l, c],
            device_id={"tp": 1 - tp},
            device_id_type=MESH,
        )

    def gate(l, c):
        need("gain")
        if l == 0:
            need(("x", c))
        need(("wv", l), ("wg", l))
        width = x_v.shape[1]
        step = width // 4
        squares = both = 0.0
        for k in range(0, width, step):
            x = x_v[own_rows(c), k : k + step].astype(jnp.float32)
            squares = squares + jnp.sum(x * x, axis=-1, keepdims=True)
            gained = (x * gain_v[l : l + 1, k : k + step]).astype(jnp.bfloat16)
            both = both + jnp.dot(gained, w_v[l, k : k + step, :], preferred_element_type=jnp.float32)
        both = both * lax.rsqrt(squares / width + 1e-06)
        a, b = plan.chunks[c]
        gated[l, a:b, :] = (both[:, :half] * jax.nn.sigmoid(both[:, half:])).astype(jnp.bfloat16)

    def send(l, c):
        for i, piece in enumerate(plan.pieces):
            if piece[0] == c:
                @pl.when(sp + piece[1] < plan.n_sp)
                def _():
                    piece_copy(l, i).start()

    def transform_taps(l):
        need("oft", "taps")
        for j in range(plan.parts):
            first = (plan.parts - 1 - j) * BLOCK
            kernels[l, j] = jnp.dot(
                oft_v[...], taps_v[l, first : first + BLOCK, :], preferred_element_type=jnp.float32
            )

    arrived = set()

    def spectrum(l, w):
        first, last = w * BLOCK, (w + 2) * BLOCK
        for i, (_, hop, _, target, count) in enumerate(plan.pieces):
            if (l, i) not in arrived and target < last and target + count > first:
                arrived.add((l, i))
                @pl.when(sp >= hop)
                def _():
                    piece_copy(l, i).wait_recv()
        need("fwd")
        spectra[w] = jnp.dot(fwd_v[...], gated[l, first:last, :], preferred_element_type=jnp.float32)

    def convolve(l, c):
        p = plan.outs - 1 - c
        tile = 16

        def bins(k, carry):
            low = pl.ds(pl.multiple_of(k * tile, tile), tile)
            high = pl.ds(pl.multiple_of(BLOCK + k * tile, tile), tile)
            real = imag = None
            for j in range(plan.parts):
                w = plan.parts - 1 + p - j
                xr, xi = spectra[w, low, :], spectra[w, high, :]
                hr, hi = kernels[l, j, low, :], kernels[l, j, high, :]
                r, i = xr * hr - xi * hi, xr * hi + xi * hr
                real, imag = (r, i) if real is None else (real + r, imag + i)
            freq[low, :] = real.astype(jnp.bfloat16)
            freq[high, :] = imag.astype(jnp.bfloat16)
            return carry

        lax.fori_loop(0, BLOCK // tile, bins, 0)
        need("inv", "bias")
        a, b = plan.chunks[c]
        result = jnp.dot(inv_v[BLOCK - (b - a) :, :], freq[...], preferred_element_type=jnp.float32)
        conv[l, tp, own_rows(c), :] = (result + bias_v[l : l + 1, :]).astype(jnp.bfloat16)
        swap_copy(l, c).start()

    def finish(l, c):
        rows = own_rows(c)
        swap_copy(l, c).wait()
        need("cgain", "cshift", ("wo", l))
        values = jnp.concatenate([conv[l, 0, rows, :], conv[l, 1, rows, :]], axis=-1).astype(jnp.float32)
        center = jnp.mean(values, axis=-1, keepdims=True)
        values = values - center
        spread = jnp.mean(values * values, axis=-1, keepdims=True)
        normed = values * lax.rsqrt(spread + 1e-05) * cgain_v[l : l + 1, :] + cshift_v[l : l + 1, :]
        mixed = (normed * jax.nn.sigmoid(normed)).astype(jnp.bfloat16)
        width = x_v.shape[1]
        step = width // 4
        for n in range(0, width, step):
            update = jnp.dot(mixed, wo_v[l, :, n : n + step], preferred_element_type=jnp.float32)
            old = x_v[rows, n : n + step].astype(jnp.float32)
            x_v[rows, n : n + step] = (old + update).astype(jnp.bfloat16)

    for c in range(plan.outs):
        gate(0, c)
        if c == 0:
            pl.semaphore_wait(barrier, 1 + jnp.minimum(plan.n_sp - 1 - sp, len(hops)))
        send(0, c)
    transform_taps(0)
    for l in range(layers):
        last = l == layers - 1
        windows = plan.parts + plan.outs - 1
        done = windows

        def after(c):
            finish(l, c)
            if not last:
                gate(l + 1, c)
                send(l + 1, c)

        finished = 0
        for c in range(plan.outs):
            while done > plan.outs - 1 - c:
                done -= 1
                spectrum(l, done)
            convolve(l, c)
            if c == 0 and not last:
                transform_taps(l + 1)
            if last:
                due = c + 1 if c < plan.outs - 2 else 0
            else:
                due = max(c, 1)
            while finished < due:
                after(finished)
                finished += 1
        while finished < plan.outs:
            after(finished)
            finished += 1

    for l in range(layers):
        for i, piece in enumerate(plan.pieces):
            @pl.when(sp + piece[1] < plan.n_sp)
            def _():
                piece_copy(l, i).wait_send()


def per_device(stream, norm_gain, value_weight, gate_weight, conv_taps, conv_bias, channel_gain, channel_shift, out_weight):
    tokens, width = stream.shape
    layers, reach, half = conv_taps.shape
    plan = Plan(tokens, width, reach, lax.axis_size("sp"))
    mats = dft_matrices(BLOCK)
    channels = out_weight.shape[1]
    n_pieces = len(plan.pieces)
    bf16, f32, dma = jnp.bfloat16, jnp.float32, pltpu.SemaphoreType.DMA
    windows = plan.parts + plan.outs - 1
    return pl.pallas_call(
        functools.partial(kernel, plan, layers),
        out_shape=pltpu.VMEM(stream.shape, stream.dtype),
        in_specs=[pl.BlockSpec(memory_space=pltpu.HBM)] * 12,
        out_specs=pl.BlockSpec(memory_space=pltpu.VMEM),
        scratch_shapes=[
            pltpu.VMEM(norm_gain.shape, f32),
            pltpu.VMEM((layers, width, 2 * half), bf16),
            pltpu.VMEM(conv_taps.shape, bf16),
            pltpu.VMEM(conv_bias.shape, f32),
            pltpu.VMEM(channel_gain.shape, f32),
            pltpu.VMEM(channel_shift.shape, f32),
            pltpu.VMEM(out_weight.shape, bf16),
            *[pltpu.VMEM(m.shape, bf16) for m in mats],
            pltpu.VMEM((layers, plan.rows, half), bf16),
            pltpu.VMEM((windows, 2 * BLOCK, half), f32),
            pltpu.VMEM((layers, plan.parts, 2 * BLOCK, half), f32),
            pltpu.VMEM((2 * BLOCK, half), bf16),
            pltpu.VMEM((layers, channels // half, tokens, half), bf16),
            dma((8 + plan.outs + 3 * layers,)),
            dma((layers, n_pieces)),
            dma((layers, n_pieces)),
            dma((layers, plan.outs)),
            dma((layers, plan.outs)),
        ],
        compiler_params=pltpu.CompilerParams(
            collective_id=0, has_side_effects=True, vmem_limit_bytes=60000 * 1024
        ),
    )(stream, norm_gain, value_weight, gate_weight, conv_taps, conv_bias, channel_gain, channel_shift, out_weight, *mats)


def solution(mesh):
    return jax.shard_map(
        per_device,
        mesh=mesh,
        in_specs=(
            P("sp", None),
            P(),
            P(None, None, "tp"),
            P(None, None, "tp"),
            P(None, None, "tp"),
            P(None, "tp"),
            P(),
            P(),
            P(),
        ),
        out_specs=P("sp", None),
        check_vma=False,
    )
```

```python
import functools

import jax
import jax.numpy as jnp
import numpy as np
from jax import lax
from jax.experimental import pallas as pl
from jax.experimental.pallas import tpu as pltpu
from jax.sharding import PartitionSpec as P

BLOCK = 128
MESH = pl.DeviceIdType.MESH


def dft_matrices(block):
    span = 2 * block
    angle = 2 * np.pi / span * np.outer(np.arange(block) + 0.5, np.arange(span))
    forward = np.concatenate([np.cos(angle), -np.sin(angle)], axis=0)
    of_taps = forward[:, block - 1 :: -1]
    inverse = forward[:, block:].T / block
    return [jnp.asarray(m, jnp.bfloat16) for m in (forward, of_taps, inverse)]


class Plan:
    def __init__(self, tokens, width, reach, n_sp):
        self.tokens, self.n_sp = tokens, n_sp
        self.parts = reach // BLOCK
        self.outs = -(-tokens // BLOCK)
        self.rows = (self.parts + self.outs) * BLOCK
        self.own = self.rows - tokens
        low = self.own - reach
        self.chunks = []
        for p in reversed(range(self.outs)):
            start = (self.parts + p) * BLOCK
            self.chunks.append((max(start, self.own), start + BLOCK))
        self.pieces = []
        for c, (a, b) in enumerate(self.chunks):
            for hop in range(1, min(-(-reach // tokens), n_sp - 1) + 1):
                first, end = max(a, low + hop * tokens) - hop * tokens, b - hop * tokens
                while first < end:
                    cut = max(first, (end - 1) // BLOCK * BLOCK if end <= self.outs * BLOCK else first)
                    when = c if hop == 1 else max(c, self.outs - 2)
                    self.pieces.append((when, hop, cut + hop * tokens, cut, end - cut))
                    end = cut
        self.pieces.sort(key=lambda piece: piece[:2])


def kernel(
    plan, layers, stream, gain, wv, wg, taps, bias, cgain, cshift, wo, fwd, oft, inv, x_v,
    gain_v, w_v, taps_v, bias_v, cgain_v, cshift_v, wo_v, fwd_v, oft_v, inv_v,
    gated, spectra, kernels, freq, conv, load_sem, send_sem, recv_sem, swap_send, swap_recv,
):
    sp, tp = lax.axis_index("sp"), lax.axis_index("tp")
    half = wv.shape[2]
    loads = {}

    def load(name, source, target):
        copy = pltpu.make_async_copy(source, target, load_sem.at[len(loads)])
        loads[name] = copy
        copy.start()

    waited = set()

    def need(*names):
        for name in names:
            if name not in waited:
                waited.add(name)
                loads[name].wait()

    def own_rows(c):
        a, b = plan.chunks[c]
        return pl.ds(a - plan.own, b - a)

    load("gain", gain, gain_v)
    load(("x", 0), stream.at[own_rows(0)], x_v.at[own_rows(0)])
    load(("wv", 0), wv.at[0], w_v.at[0, :, pl.ds(0, half)])
    load(("wg", 0), wg.at[0], w_v.at[0, :, pl.ds(half, half)])
    for c in range(1, plan.outs):
        load(("x", c), stream.at[own_rows(c)], x_v.at[own_rows(c)])
    load("oft", oft, oft_v)
    load("taps", taps, taps_v)
    load("fwd", fwd, fwd_v)
    load("inv", inv, inv_v)
    load("bias", bias, bias_v)
    load("cgain", cgain, cgain_v)
    load("cshift", cshift, cshift_v)
    load(("wo", 0), wo.at[0], wo_v.at[0])
    for l in range(1, layers):
        load(("wv", l), wv.at[l], w_v.at[l, :, pl.ds(0, half)])
        load(("wg", l), wg.at[l], w_v.at[l, :, pl.ds(half, half)])
        load(("wo", l), wo.at[l], wo_v.at[l])

    for l in range(layers):
        gated[l, : plan.own] = jnp.zeros((plan.own, half), jnp.bfloat16)

    hops = sorted({piece[1] for piece in plan.pieces})
    barrier = pltpu.get_barrier_semaphore()
    pl.semaphore_signal(barrier, inc=1, device_id={"tp": 1 - tp}, device_id_type=MESH)
    for hop in hops:
        @pl.when(sp >= hop)
        def _():
            pl.semaphore_signal(barrier, inc=1, device_id={"sp": sp - hop}, device_id_type=MESH)

    def piece_copy(l, i):
        _, hop, source, target, count = plan.pieces[i]
        return pltpu.make_async_remote_copy(
            src_ref=gated.at[l, pl.ds(source, count)],
            dst_ref=gated.at[l, pl.ds(target, count)],
            send_sem=send_sem.at[l, i],
            recv_sem=recv_sem.at[l, i],
            device_id={"sp": sp + hop},
            device_id_type=MESH,
        )

    def swap_copy(l, c):
        part = conv.at[l, tp, own_rows(c)]
        return pltpu.make_async_remote_copy(
            src_ref=part,
            dst_ref=part,
            send_sem=swap_send.at[l, c],
            recv_sem=swap_recv.at[l, c],
            device_id={"tp": 1 - tp},
            device_id_type=MESH,
        )

    def gate(l, c):
        need("gain")
        if l == 0:
            need(("x", c))
        need(("wv", l), ("wg", l))
        width = x_v.shape[1]
        step = width // 4
        squares = both = 0.0
        for k in range(0, width, step):
            x = x_v[own_rows(c), k : k + step].astype(jnp.float32)
            squares = squares + jnp.sum(x * x, axis=-1, keepdims=True)
            gained = (x * gain_v[l : l + 1, k : k + step]).astype(jnp.bfloat16)
            both = both + jnp.dot(gained, w_v[l, k : k + step, :], preferred_element_type=jnp.float32)
        both = both * lax.rsqrt(squares / width + 1e-06)
        a, b = plan.chunks[c]
        gated[l, a:b, :] = (both[:, :half] * jax.nn.sigmoid(both[:, half:])).astype(jnp.bfloat16)

    def send(l, c):
        for i, piece in enumerate(plan.pieces):
            if piece[0] == c:
                @pl.when(sp + piece[1] < plan.n_sp)
                def _():
                    piece_copy(l, i).start()

    def transform_taps(l):
        need("oft", "taps")
        for j in range(plan.parts):
            first = (plan.parts - 1 - j) * BLOCK
            kernels[l, j] = jnp.dot(
                oft_v[...], taps_v[l, first : first + BLOCK, :], preferred_element_type=jnp.float32
            )

    arrived = set()

    def spectrum(l, w):
        first, last = w * BLOCK, (w + 2) * BLOCK
        for i, (_, hop, _, target, count) in enumerate(plan.pieces):
            if (l, i) not in arrived and target < last and target + count > first:
                arrived.add((l, i))
                @pl.when(sp >= hop)
                def _():
                    piece_copy(l, i).wait_recv()
        need("fwd")
        spectra[w] = jnp.dot(fwd_v[...], gated[l, first:last, :], preferred_element_type=jnp.float32)

    def convolve(l, c):
        p = plan.outs - 1 - c
        tile = 16

        def bins(k, carry):
            low = pl.ds(pl.multiple_of(k * tile, tile), tile)
            high = pl.ds(pl.multiple_of(BLOCK + k * tile, tile), tile)
            real = imag = None
            for j in range(plan.parts):
                w = plan.parts - 1 + p - j
                xr, xi = spectra[w, low, :], spectra[w, high, :]
                hr, hi = kernels[l, j, low, :], kernels[l, j, high, :]
                r, i = xr * hr - xi * hi, xr * hi + xi * hr
                real, imag = (r, i) if real is None else (real + r, imag + i)
            freq[low, :] = real.astype(jnp.bfloat16)
            freq[high, :] = imag.astype(jnp.bfloat16)
            return carry

        lax.fori_loop(0, BLOCK // tile, bins, 0)
        need("inv", "bias")
        a, b = plan.chunks[c]
        result = jnp.dot(inv_v[BLOCK - (b - a) :, :], freq[...], preferred_element_type=jnp.float32)
        conv[l, tp, own_rows(c), :] = (result + bias_v[l : l + 1, :]).astype(jnp.bfloat16)
        swap_copy(l, c).start()

    def finish(l, c):
        rows = own_rows(c)
        swap_copy(l, c).wait()
        need("cgain", "cshift", ("wo", l))
        values = jnp.concatenate([conv[l, 0, rows, :], conv[l, 1, rows, :]], axis=-1).astype(jnp.float32)
        center = jnp.mean(values, axis=-1, keepdims=True)
        values = values - center
        spread = jnp.mean(values * values, axis=-1, keepdims=True)
        normed = values * lax.rsqrt(spread + 1e-05) * cgain_v[l : l + 1, :] + cshift_v[l : l + 1, :]
        mixed = (normed * jax.nn.sigmoid(normed)).astype(jnp.bfloat16)
        width = x_v.shape[1]
        step = width // 4
        for n in range(0, width, step):
            update = jnp.dot(mixed, wo_v[l, :, n : n + step], preferred_element_type=jnp.float32)
            old = x_v[rows, n : n + step].astype(jnp.float32)
            x_v[rows, n : n + step] = (old + update).astype(jnp.bfloat16)

    for c in range(plan.outs):
        gate(0, c)
        if c == 0:
            pl.semaphore_wait(barrier, 1 + jnp.minimum(plan.n_sp - 1 - sp, len(hops)))
        send(0, c)
    transform_taps(0)
    for l in range(layers):
        last = l == layers - 1
        windows = plan.parts + plan.outs - 1
        done = windows

        def after(c):
            finish(l, c)
            if not last:
                gate(l + 1, c)
                send(l + 1, c)

        finished = 0
        for c in range(plan.outs):
            while done > plan.outs - 1 - c:
                done -= 1
                spectrum(l, done)
            convolve(l, c)
            if c == 0 and not last:
                transform_taps(l + 1)
            due = c
            while finished < due:
                after(finished)
                finished += 1
        while finished < plan.outs:
            after(finished)
            finished += 1

    for l in range(layers):
        for i, piece in enumerate(plan.pieces):
            @pl.when(sp + piece[1] < plan.n_sp)
            def _():
                piece_copy(l, i).wait_send()


def per_device(stream, norm_gain, value_weight, gate_weight, conv_taps, conv_bias, channel_gain, channel_shift, out_weight):
    tokens, width = stream.shape
    layers, reach, half = conv_taps.shape
    plan = Plan(tokens, width, reach, lax.axis_size("sp"))
    mats = dft_matrices(BLOCK)
    channels = out_weight.shape[1]
    n_pieces = len(plan.pieces)
    bf16, f32, dma = jnp.bfloat16, jnp.float32, pltpu.SemaphoreType.DMA
    windows = plan.parts + plan.outs - 1
    return pl.pallas_call(
        functools.partial(kernel, plan, layers),
        out_shape=pltpu.VMEM(stream.shape, stream.dtype),
        in_specs=[pl.BlockSpec(memory_space=pltpu.HBM)] * 12,
        out_specs=pl.BlockSpec(memory_space=pltpu.VMEM),
        scratch_shapes=[
            pltpu.VMEM(norm_gain.shape, f32),
            pltpu.VMEM((layers, width, 2 * half), bf16),
            pltpu.VMEM(conv_taps.shape, bf16),
            pltpu.VMEM(conv_bias.shape, f32),
            pltpu.VMEM(channel_gain.shape, f32),
            pltpu.VMEM(channel_shift.shape, f32),
            pltpu.VMEM(out_weight.shape, bf16),
            *[pltpu.VMEM(m.shape, bf16) for m in mats],
            pltpu.VMEM((layers, plan.rows, half), bf16),
            pltpu.VMEM((windows, 2 * BLOCK, half), f32),
            pltpu.VMEM((layers, plan.parts, 2 * BLOCK, half), f32),
            pltpu.VMEM((2 * BLOCK, half), bf16),
            pltpu.VMEM((layers, channels // half, tokens, half), bf16),
            dma((8 + plan.outs + 3 * layers,)),
            dma((layers, n_pieces)),
            dma((layers, n_pieces)),
            dma((layers, plan.outs)),
            dma((layers, plan.outs)),
        ],
        compiler_params=pltpu.CompilerParams(
            collective_id=0, has_side_effects=True, vmem_limit_bytes=60000 * 1024
        ),
    )(stream, norm_gain, value_weight, gate_weight, conv_taps, conv_bias, channel_gain, channel_shift, out_weight, *mats)


def solution(mesh):
    return jax.shard_map(
        per_device,
        mesh=mesh,
        in_specs=(
            P("sp", None),
            P(),
            P(None, None, "tp"),
            P(None, None, "tp"),
            P(None, None, "tp"),
            P(None, "tp"),
            P(),
            P(),
            P(),
        ),
        out_specs=P("sp", None),
        check_vma=False,
    )
```
